768 devices in a mesh: fs: 24 (over z, core), tp: 32 (over y, x).
Axes of the slice: x: 4, y: 8, z: 12, core: 2. Of those that a mesh axis runs over, the one named last changes fastest.
Arguments:
- tokens: bfloat16 [4608, 2304], P('fs'), may hold values from -6 to 6
- gate_train: float32 [8, 2304, 2304], P(None, 'fs', 'tp'), may hold values from -0.125 to 0.125
- up_train: float32 [8, 2304, 2304], P(None, 'fs', 'tp'), may hold values from -0.125 to 0.125
- down_train: float32 [8, 2304, 2304], P(None, 'fs', 'tp'), may hold values from -0.125 to 0.125
- gain: float32 [2304], P('fs'), may hold values from 0.1 to 1.9
- routes: int32 [4608, 2], P('fs'), may hold values from 0 to 7, all different within a row; in each aligned block of 192 rows (0 to 191, 192 to 383, ...) at most 72 rows name the same one
- route_weights: float32 [4608, 2], P('fs'), may hold values from 0.1 to 1
Outputs:
- gate_new: bfloat16 [32, 576, 2304], P('tp')
- up_new: bfloat16 [32, 576, 2304], P('tp')
- down_new: bfloat16 [32, 576, 2304], P('tp')
- mixed: bfloat16 [4608, 2304], P('fs', 'tp')
The draws below stay inside these ranges and needn't reach their ends.
Inputs may be any that keep to these rules, and one draw needn't show every extreme that they name: `routes`: each row names two different experts; in each aligned block of 192 rows at most 72 rows name one expert, a bound that some block reaches.
All inputs are finite; a program needn't handle non-finite values.
Results may differ from the reference program's by a relative error of at most 0.0095.
Values may be sent and summed in bfloat16 or wider, within the bound.
No kernel may reach another device: no remote copies, remote signals or barrier semaphores. Data moves between devices by JAX's collectives and lax.ppermute only.
A program may use at most 64 MiB of HBM per device.

```python
import math
import jax
import jax.numpy as jnp
import numpy as np
from jax import lax

D = 2304
FF = 2304
EXPERTS = 8
ROWS = 192
CAP = 72
TOKENS = 4608
N_FS = 24
N_TP = 32


def levels(own_key, shape, pieces, smallest, largest):
    level, own = 1.0, jax.random.fold_in(own_key, 6)
    for position, shards_of in pieces:
        heights = jnp.exp(jax.random.uniform(jax.random.fold_in(own, position), (shards_of,), jnp.float32, smallest / len(pieces), largest / len(pieces)))
        level = level * jnp.repeat(heights, shape[position] // shards_of).reshape([-1 if axis == position else 1 for axis in range(len(shape))])
    return level


def routed_block(own_key, own, number, rows, number_of, top, most, lean):
    sequence = jax.random.permutation(own_key, number_of)
    packed, usual = load_shares(number_of, rows * top, most, lean, True), load_shares(number_of, rows * top, most, lean, False)
    places = jnp.arange(number_of)

    def named(lengths, rotation):
        used = int((lengths > 0).sum())
        fixed = max(1, used // 4)
        passed = fixed + (places - fixed + rotation * (used - fixed)) % max(1, number_of - fixed)
        return jnp.zeros((number_of,), jnp.int32).at[sequence[jnp.where(places < fixed, places, passed)]].set(jnp.asarray(lengths, jnp.int32))

    lengths = jnp.where(number % 4 == 0, named(packed, number // 4), named(usual, number - number // 4 - 1))
    mixed = jax.random.permutation(jax.random.fold_in(own, 3), number_of)
    giver, receiver = mixed[0:number_of // 2 * 2:2], mixed[1:number_of // 2 * 2:2]
    margin = jnp.minimum(lengths[giver] - 1, most - lengths[receiver]) // 2
    margin = jnp.where((giver == sequence[0]) | (receiver == sequence[0]) | (lengths[receiver] == 0), 0, jnp.maximum(margin, 0))
    passed = jax.random.randint(jax.random.fold_in(own, 4), (number_of // 2,), 0, 1 << 20) % (margin + 1)
    lengths = lengths.at[giver].add(-passed).at[receiver].add(passed)
    members = jnp.searchsorted(jnp.cumsum(lengths), jnp.arange(rows * top), side="right").astype(jnp.int32)
    table = members.reshape(top, rows).T
    table = table[jax.random.permutation(jax.random.fold_in(own, 1), rows)]
    rotation = jax.random.randint(jax.random.fold_in(own, 2), (rows, 1), 0, top)
    return jnp.take_along_axis(table, (jnp.arange(top)[None, :] + rotation) % top, axis=1)


def load_shares(count, total, bound, skew, full):
    loads = [(1 << 20) // math.isqrt(rank ** skew) + 1 for rank in range(1, count + 1)]
    largest = bound if full else min(bound, max(-(-total // count), total * loads[0] // sum(loads)))
    least = 1 if total - largest >= count - 1 else 0
    given, rest = [largest] + [least] * (count - 1), total - largest - least * (count - 1)
    while rest > 0:
        free = [i for i in range(1, count) if given[i] < largest] or [i for i in range(1, count) if given[i] < bound]
        pool, remaining = sum([loads[i] for i in free]), rest
        for i in free:
            extra = min(bound - given[i], max(1, remaining * loads[i] // pool), rest)
            given[i] = given[i] + extra
            rest = rest - extra
    return np.array(given)


def scatter_about(stream_key, shape, scale, bound, split=(), kind=jnp.bfloat16):
    array = scale * jax.random.normal(stream_key, shape, jnp.float32)
    if split:
        array = array * levels(stream_key, shape, split, -0.22, 0.18)
    return jnp.clip(array, -bound, bound).astype(kind)


def setup_inputs(seed: int = 0) -> dict:
    keys = jax.random.split(jax.random.key(seed), 8)
    tokens = scatter_about(keys[0], (TOKENS, D), 1.0, 6.0, ((0, 24),))
    gate_train = scatter_about(keys[1], (EXPERTS, D, FF), D ** -0.5, 0.125, ((1, 24), (2, 32)), jnp.float32)
    up_train = scatter_about(keys[2], (EXPERTS, D, FF), D ** -0.5, 0.125, ((1, 24), (2, 32)), jnp.float32)
    down_train = scatter_about(keys[3], (EXPERTS, D, FF), FF ** -0.5, 0.125, ((1, 24), (2, 32)), jnp.float32)
    gain = jnp.clip(1.0 + 0.18 * jax.random.normal(keys[4], (D,), jnp.float32), 0.1, 1.9)
    routes_keys = jax.random.split(jax.random.fold_in(keys[5], 1), TOKENS // ROWS)
    routes_turns = jax.random.permutation(jax.random.fold_in(keys[5], 3), TOKENS // ROWS)
    routes = jax.vmap(lambda own, number: routed_block(jax.random.fold_in(keys[5], 2), own, number, ROWS, EXPERTS, 2, CAP, 1))(routes_keys, routes_turns).reshape((TOKENS, 2))
    route_weights = jnp.clip(0.1 + 0.9 * jax.random.uniform(keys[6], (TOKENS, 2), jnp.float32) ** levels(keys[6], (TOKENS, 2), ((0, 24),), -0.2, 0.2), 0.1, 1.0)
    return dict(tokens=tokens, gate_train=gate_train, up_train=up_train, down_train=down_train, gain=gain, routes=routes, route_weights=route_weights)


norm_eps = 1e-06

def arrange(matrix):
    experts, row_count, col_count = matrix.shape
    slices = N_TP // experts
    piece_width = col_count // (N_TP * slices)
    shaped = matrix.reshape(experts, row_count, N_TP, slices, piece_width)
    return shaped.transpose(0, 3, 2, 4, 1).reshape(experts * slices, col_count // slices, row_count)

def reference(tokens, gate_train, up_train, down_train, gain, routes, route_weights):
    gain_column = gain.astype(jnp.float32)[None, :, None]
    gate_new = arrange((gate_train * gain_column).astype(jnp.bfloat16))
    up_new = arrange((up_train * gain_column).astype(jnp.bfloat16))
    down_new = arrange(down_train.astype(jnp.bfloat16))
    tokens_wide = tokens.astype(jnp.float32)
    normed = (tokens_wide * lax.rsqrt(lax.optimization_barrier(jnp.mean(tokens_wide * tokens_wide, axis=1, keepdims=True)) + norm_eps)).astype(jnp.bfloat16)
    slices = N_TP // EXPERTS

    def one_block(inputs):
        block_rows, block_routes, block_weights = inputs

        def per_expert(expert, output):
            matches = block_routes == expert
            member = jnp.any(matches, axis=1)
            slot_index = (jnp.cumsum(member.astype(jnp.int32)) - 1).astype(jnp.int32)
            marked = jnp.where(member, slot_index, -1)
            picker = (marked[None, :] == jnp.arange(CAP, dtype=jnp.int32)[:, None]).astype(jnp.bfloat16)
            chosen = jnp.dot(picker, block_rows, preferred_element_type=jnp.float32).astype(jnp.bfloat16)
            gate_part = lax.dynamic_slice_in_dim(gate_new, expert * slices, slices, 0).astype(jnp.float32)
            up_part = lax.dynamic_slice_in_dim(up_new, expert * slices, slices, 0).astype(jnp.float32)
            down_part = lax.dynamic_slice_in_dim(down_new, expert * slices, slices, 0).astype(jnp.float32)
            chosen_wide = chosen.astype(jnp.float32)
            gate_pre = jnp.einsum('cd,sfd->scf', chosen_wide, gate_part)
            up_pre = jnp.einsum('cd,sfd->scf', chosen_wide, up_part)
            hidden = (jax.nn.silu(gate_pre) * up_pre).astype(jnp.bfloat16)
            partial_value = jnp.einsum('scf,sfd->scd', hidden.astype(jnp.float32), down_part).astype(jnp.bfloat16)
            slice_total = lax.optimization_barrier(jnp.sum(partial_value.astype(jnp.float32), axis=0))
            row_weight = lax.optimization_barrier(jnp.sum(jnp.where(matches, block_weights, 0.0), axis=1))
            gathered = jnp.take(slice_total, jnp.clip(slot_index, 0, CAP - 1), axis=0)
            return output + jnp.where(member[:, None], row_weight[:, None] * gathered, 0.0)
        return lax.fori_loop(0, EXPERTS, per_expert, jnp.zeros((ROWS, D), jnp.float32)).astype(jnp.bfloat16)
    mixed = lax.map(one_block, (normed.reshape(N_FS, ROWS, D), routes.reshape(N_FS, ROWS, 2), route_weights.reshape(N_FS, ROWS, 2)))
    return (gate_new, up_new, down_new, mixed.reshape(TOKENS, D))
```

```python
import jax
import jax.numpy as jnp
from jax import lax
from jax.experimental import pallas as pl
from jax.experimental.pallas import tpu as pltpu
from jax.sharding import PartitionSpec as P

CAP = 72
EPS = 1e-06
STEPS = (56, 28, 14, 8, 4, 2, 1)
LAST = (((1,), (1,)), ((), ()))


def arrange(matrix, tp_count):
    experts, rows, cols = matrix.shape
    slices = tp_count // experts
    turned = matrix.transpose(0, 2, 1)
    return turned.reshape(tp_count, cols // slices, rows)


def ranks(routes_t, experts):
    rows = routes_t.shape[1]
    labels = lax.broadcasted_iota(jnp.int32, (experts, rows), 0)
    first = routes_t[0:1, :] == labels
    second = routes_t[1:2, :] == labels
    member = jnp.where(first | second, 1.0, 0.0)
    before = lax.broadcasted_iota(jnp.int32, (rows, rows), 0) < lax.broadcasted_iota(
        jnp.int32, (rows, rows), 1
    )
    earlier = jnp.where(before, 1.0, 0.0).astype(jnp.bfloat16)
    rank = jnp.dot(member.astype(jnp.bfloat16), earlier, preferred_element_type=jnp.float32)
    return member, rank


def choose_kernel(expert_ref, tokens_ref, routes_ref, chosen_ref):
    wide = tokens_ref[...].astype(jnp.float32)
    scale = lax.rsqrt(jnp.mean(wide * wide, axis=1, keepdims=True) + EPS)
    normed = (wide * scale).astype(jnp.bfloat16)
    rows = wide.shape[0]
    member, rank = ranks(routes_ref[...], 8)
    own = lax.broadcasted_iota(jnp.int32, member.shape, 0) == expert_ref[0]
    marked = jnp.where(own & (member > 0.5), rank, -1.0)
    place = jnp.sum(jnp.where(own, marked, 0.0), axis=0, keepdims=True)
    slots = lax.broadcasted_iota(jnp.int32, (CAP, rows), 0).astype(jnp.float32)
    picker = jnp.where(slots == place, 1.0, 0.0).astype(jnp.bfloat16)
    chosen_ref[...] = jnp.dot(picker, normed, preferred_element_type=jnp.float32).astype(
        jnp.bfloat16
    )


def unpack(block_ref, start, out_ref):
    rows = out_ref.shape[0] // 4
    lanes = out_ref.shape[1]
    width = lanes // 4
    place = lax.broadcasted_iota(jnp.int32, (rows, lanes), 1)
    parts = [block_ref[s, start : start + rows, :] for s in range(4)]
    for g in range(4):
        merged = parts[(3 - g) % 4]
        for p in (2, 1, 0):
            merged = jnp.where(place < (p + 1) * width, parts[(p - g) % 4], merged)
        if g:
            merged = jnp.concatenate([merged[:, g * width :], merged[:, : g * width]], axis=1)
        out_ref[g * rows : (g + 1) * rows, :] = merged


def first_kernel(block_ref, chosen_ref, gate_ref, up_ref, hidden_ref, gate_sum, up_sum):
    step = pl.program_id(0)

    @pl.when(step == 0)
    def _():
        gate_sum[...] = jnp.zeros_like(gate_sum)
        up_sum[...] = jnp.zeros_like(up_sum)

    rows = gate_ref.shape[0] // 4
    unpack(block_ref, 0, gate_ref)
    unpack(block_ref, rows, up_ref)
    chosen = chosen_ref[...]
    gate_sum[...] += lax.dot_general(
        chosen, gate_ref[...], LAST, preferred_element_type=jnp.float32
    )
    up_sum[...] += lax.dot_general(chosen, up_ref[...], LAST, preferred_element_type=jnp.float32)

    @pl.when(step == pl.num_programs(0) - 1)
    def _():
        gate = gate_sum[...]
        hidden_ref[...] = (gate / (1.0 + jnp.exp(-gate)) * up_sum[...]).astype(jnp.bfloat16)


def second_kernel(block_ref, hidden_ref, down_ref, partial_ref):
    unpack(block_ref, 0, down_ref)
    product = jnp.dot(hidden_ref[...], down_ref[...], preferred_element_type=jnp.float32)
    partial_ref[...] = product.T.astype(jnp.bfloat16)


def combine_kernel(received_ref, routes_ref, weights_ref, mixed_ref):
    experts = 8
    slices = received_ref.shape[0] // experts
    routes = routes_ref[...]
    rows = routes.shape[1]
    _, rank = ranks(routes, experts)
    width = received_ref.shape[1]
    slots = lax.broadcasted_iota(jnp.int32, (CAP, rows), 0).astype(jnp.float32)
    totals = [jnp.zeros((width, rows), jnp.float32) for _ in range(2)]
    for e in range(experts):
        summed = received_ref[e * slices].astype(jnp.float32)
        for s in range(1, slices):
            summed = summed + received_ref[e * slices + s].astype(jnp.float32)
        high = summed.astype(jnp.bfloat16)
        low = (summed - high.astype(jnp.float32)).astype(jnp.bfloat16)
        at = slots == rank[e : e + 1, :]
        for j in range(2):
            named = routes[j : j + 1, :] == e
            pick = jnp.where(at & named, 1.0, 0.0).astype(jnp.bfloat16)
            totals[j] = (
                totals[j]
                + jnp.dot(high, pick, preferred_element_type=jnp.float32)
                + jnp.dot(low, pick, preferred_element_type=jnp.float32)
            )
    weights = weights_ref[...]
    mixed_ref[...] = (weights[0:1, :] * totals[0] + weights[1:2, :] * totals[1]).astype(
        jnp.bfloat16
    )


def shards(tokens, gate_train, up_train, down_train, gain, routes, route_weights):
    tp_count = lax.axis_size("tp")
    fs_count = lax.axis_size("fs")
    experts, features, _ = gate_train.shape
    slices = tp_count // experts
    gain_column = gain[None, :, None]
    gate_round = (gate_train * gain_column).astype(jnp.bfloat16)
    up_round = (up_train * gain_column).astype(jnp.bfloat16)
    down_round = down_train.astype(jnp.bfloat16)
    pieces = [arrange(a, tp_count) for a in (gate_round, up_round, down_round)]
    units = pieces[0].shape[1]
    moved = lax.all_to_all(
        jnp.concatenate(pieces, axis=1), "tp", split_axis=0, concat_axis=0, tiled=True
    )

    expert = (lax.axis_index("tp") // slices).astype(jnp.int32).reshape(1)
    routes_t = routes.T
    weights_t = route_weights.T
    rows, width = tokens.shape
    chosen = pl.pallas_call(
        choose_kernel,
        out_shape=jax.ShapeDtypeStruct((CAP, width), jnp.bfloat16),
        in_specs=[
            pl.BlockSpec(memory_space=pltpu.SMEM),
            pl.BlockSpec(memory_space=pltpu.VMEM),
            pl.BlockSpec(memory_space=pltpu.VMEM),
        ],
        out_specs=pl.BlockSpec(memory_space=pltpu.VMEM),
        cost_estimate=pl.CostEstimate(flops=2000000000, bytes_accessed=2000000, transcendentals=0),
    )(expert, tokens, routes_t)

    block_rows = tp_count * units
    quarter = block_rows // 4
    grouped = jnp.stack(
        [
            moved[:, m * units : (m + 1) * units].reshape(4, quarter, features)
            for m in range(3)
        ],
        axis=1,
    )
    shift = (4 - lax.axis_index("fs") % 4) % 4
    turned = lax.dynamic_slice_in_dim(jnp.concatenate([grouped, grouped], axis=0), shift, 4, 0)
    packed = jnp.concatenate([turned[p] for p in range(4)], axis=-1)
    lanes = 4 * features

    wide = packed.astype(jnp.float32)
    largest = jnp.max(jnp.abs(wide), axis=(1, 2))
    factor = jnp.ones_like(largest)
    power = jnp.zeros_like(largest)
    for b in STEPS:
        fits = largest * factor * 2.0**b <= 32768.0
        factor = jnp.where(fits, factor * 2.0**b, factor)
        power = jnp.where(fits, power + b, power)
    sent = (wide * factor[:, None, None]).astype(jnp.float16).reshape(3 * quarter, lanes)
    note = jnp.broadcast_to(power[:, None], (3, lanes // 3)).reshape(1, lanes)
    note = jnp.broadcast_to(note, (8, lanes)).astype(jnp.float16)
    gathered = lax.all_gather(jnp.concatenate([sent, note], axis=0), "fs", axis=0)
    left = jnp.stack(
        [gathered[:, 3 * quarter, m * (lanes // 3)] for m in range(3)], axis=1
    ).astype(jnp.float32)
    back = jnp.ones_like(left)
    for b in STEPS:
        holds = left >= b
        back = jnp.where(holds, back * 2.0**-b, back)
        left = jnp.where(holds, left - b, left)

    def returned(start, stop):
        part = gathered[:, start * quarter : stop * quarter].astype(jnp.float32)
        part = part.reshape(fs_count, stop - start, quarter, lanes)
        part = (part * back[:, start:stop, None, None]).astype(jnp.bfloat16)
        return part.reshape(fs_count, (stop - start) * quarter, lanes)

    both = returned(0, 2)
    third = returned(2, 3)
    steps = fs_count // 4
    matrix = jax.ShapeDtypeStruct((block_rows, width), jnp.bfloat16)
    matrix_spec = pl.BlockSpec((block_rows, lanes), lambda i: (0, i))
    gate_new, up_new, hidden = pl.pallas_call(
        first_kernel,
        grid=(steps,),
        out_shape=(matrix, matrix, jax.ShapeDtypeStruct((CAP, block_rows), jnp.bfloat16)),
        in_specs=[
            pl.BlockSpec((4, 2 * quarter, lanes), lambda i: (i, 0, 0)),
            pl.BlockSpec((CAP, lanes), lambda i: (0, i)),
        ],
        out_specs=(matrix_spec, matrix_spec, pl.BlockSpec((CAP, block_rows), lambda i: (0, 0))),
        scratch_shapes=[pltpu.VMEM((CAP, block_rows), jnp.float32)] * 2,
    )(both, chosen)
    down_new, partial = pl.pallas_call(
        second_kernel,
        grid=(steps,),
        out_shape=(matrix, jax.ShapeDtypeStruct((width, CAP), jnp.bfloat16)),
        in_specs=[
            pl.BlockSpec((4, quarter, lanes), lambda i: (i, 0, 0)),
            pl.BlockSpec((CAP, block_rows), lambda i: (0, 0)),
        ],
        out_specs=(matrix_spec, pl.BlockSpec((lanes, CAP), lambda i: (i, 0))),
    )(third, hidden)

    received = lax.all_to_all(
        partial.reshape(tp_count, width // tp_count, CAP),
        "tp",
        split_axis=0,
        concat_axis=0,
        tiled=True,
    )
    mixed = pl.pallas_call(
        combine_kernel,
        out_shape=jax.ShapeDtypeStruct((width // tp_count, rows), jnp.bfloat16),
    )(received, routes_t, weights_t)
    return (gate_new[None], up_new[None], down_new[None], mixed.T)


def solution(mesh):
    in_specs = (
        P("fs", None),
        P(None, "fs", "tp"),
        P(None, "fs", "tp"),
        P(None, "fs", "tp"),
        P("fs"),
        P("fs", None),
        P("fs", None),
    )
    out_specs = (P("tp", None, None), P("tp", None, None), P("tp", None, None), P("fs", "tp"))
    return jax.shard_map(shards, mesh=mesh, in_specs=in_specs, out_specs=out_specs, check_vma=False)
```

```python
import jax
import jax.numpy as jnp
from jax import lax
from jax.experimental import pallas as pl
from jax.experimental.pallas import tpu as pltpu
from jax.sharding import PartitionSpec as P

CAP = 72
EPS = 1e-06
STEPS = (56, 28, 14, 8, 4, 2, 1)
LAST = (((1,), (1,)), ((), ()))


def arrange(matrix, tp_count):
    experts, rows, cols = matrix.shape
    slices = tp_count // experts
    turned = matrix.transpose(0, 2, 1)
    return turned.reshape(tp_count, cols // slices, rows)


def ranks(routes_t, experts):
    rows = routes_t.shape[1]
    labels = lax.broadcasted_iota(jnp.int32, (experts, rows), 0)
    first = routes_t[0:1, :] == labels
    second = routes_t[1:2, :] == labels
    member = jnp.where(first | second, 1.0, 0.0)
    before = lax.broadcasted_iota(jnp.int32, (rows, rows), 0) < lax.broadcasted_iota(
        jnp.int32, (rows, rows), 1
    )
    earlier = jnp.where(before, 1.0, 0.0).astype(jnp.bfloat16)
    rank = jnp.dot(member.astype(jnp.bfloat16), earlier, preferred_element_type=jnp.float32)
    return member, rank


def choose_kernel(expert_ref, tokens_ref, routes_ref, chosen_ref):
    wide = tokens_ref[...].astype(jnp.float32)
    scale = lax.rsqrt(jnp.mean(wide * wide, axis=1, keepdims=True) + EPS)
    normed = (wide * scale).astype(jnp.bfloat16)
    rows = wide.shape[0]
    member, rank = ranks(routes_ref[...], 8)
    own = lax.broadcasted_iota(jnp.int32, member.shape, 0) == expert_ref[0]
    marked = jnp.where(own & (member > 0.5), rank, -1.0)
    place = jnp.sum(jnp.where(own, marked, 0.0), axis=0, keepdims=True)
    slots = lax.broadcasted_iota(jnp.int32, (CAP, rows), 0).astype(jnp.float32)
    picker = jnp.where(slots == place, 1.0, 0.0).astype(jnp.bfloat16)
    chosen_ref[...] = jnp.dot(picker, normed, preferred_element_type=jnp.float32).astype(
        jnp.bfloat16
    )


def unpack(block_ref, start, out_ref):
    rows = out_ref.shape[0] // 4
    lanes = out_ref.shape[1]
    width = lanes // 4
    place = lax.broadcasted_iota(jnp.int32, (rows, lanes), 1)
    parts = [block_ref[s, start : start + rows, :] for s in range(4)]
    for g in range(4):
        merged = parts[(3 - g) % 4]
        for p in (2, 1, 0):
            merged = jnp.where(place < (p + 1) * width, parts[(p - g) % 4], merged)
        if g:
            merged = jnp.concatenate([merged[:, g * width :], merged[:, : g * width]], axis=1)
        out_ref[g * rows : (g + 1) * rows, :] = merged


def product_kernel(
    both_ref,
    third_ref,
    chosen_ref,
    gate_ref,
    up_ref,
    partial_ref,
    down_ref,
    hidden_ref,
    gate_sum,
    up_sum,
):
    i = pl.program_id(0)
    steps = both_ref.shape[0] // 4
    lanes = gate_ref.shape[1]
    rows = gate_ref.shape[0] // 4

    @pl.when(i < steps)
    def _():
        unpack(both_ref.at[pl.ds(4 * i, 4)], 0, gate_ref)
        unpack(both_ref.at[pl.ds(4 * i, 4)], rows, up_ref)
        chosen = chosen_ref[:, pl.ds(pl.multiple_of(i * lanes, 128), lanes)]
        gate = lax.dot_general(chosen, gate_ref[...], LAST, preferred_element_type=jnp.float32)
        up = lax.dot_general(chosen, up_ref[...], LAST, preferred_element_type=jnp.float32)

        @pl.when(i == 0)
        def _():
            gate_sum[...] = gate
            up_sum[...] = up

        @pl.when(i > 0)
        def _():
            gate_sum[...] += gate
            up_sum[...] += up

    @pl.when(i == steps - 1)
    def _():
        total = gate_sum[...]
        hidden_ref[...] = (total / (1.0 + jnp.exp(-total)) * up_sum[...]).astype(jnp.bfloat16)

    @pl.when(i >= steps)
    def _():
        unpack(third_ref.at[pl.ds(4 * (i - steps), 4)], 0, down_ref)
        product = jnp.dot(hidden_ref[...], down_ref[...], preferred_element_type=jnp.float32)
        partial_ref[...] = product.T.astype(jnp.bfloat16)


def output_kernel(third_ref, down_ref):
    unpack(third_ref.at[pl.ds(4 * pl.program_id(0), 4)], 0, down_ref)


def combine_kernel(received_ref, routes_ref, weights_ref, mixed_ref):
    experts = 8
    slices = received_ref.shape[0] // experts
    routes = routes_ref[...]
    rows = routes.shape[1]
    _, rank = ranks(routes, experts)
    width = received_ref.shape[1]
    slots = lax.broadcasted_iota(jnp.int32, (CAP, rows), 0).astype(jnp.float32)
    totals = [jnp.zeros((width, rows), jnp.float32) for _ in range(2)]
    for e in range(experts):
        summed = received_ref[e * slices].astype(jnp.float32)
        for s in range(1, slices):
            summed = summed + received_ref[e * slices + s].astype(jnp.float32)
        high = summed.astype(jnp.bfloat16)
        low = (summed - high.astype(jnp.float32)).astype(jnp.bfloat16)
        at = slots == rank[e : e + 1, :]
        for j in range(2):
            named = routes[j : j + 1, :] == e
            pick = jnp.where(at & named, 1.0, 0.0).astype(jnp.bfloat16)
            totals[j] = (
                totals[j]
                + jnp.dot(high, pick, preferred_element_type=jnp.float32)
                + jnp.dot(low, pick, preferred_element_type=jnp.float32)
            )
    weights = weights_ref[...]
    mixed_ref[...] = (weights[0:1, :] * totals[0] + weights[1:2, :] * totals[1]).astype(
        jnp.bfloat16
    )


def shards(tokens, gate_train, up_train, down_train, gain, routes, route_weights):
    tp_count = lax.axis_size("tp")
    fs_count = lax.axis_size("fs")
    experts, features, _ = gate_train.shape
    slices = tp_count // experts
    gain_column = gain[None, :, None]
    gate_round = (gate_train * gain_column).astype(jnp.bfloat16)
    up_round = (up_train * gain_column).astype(jnp.bfloat16)
    down_round = down_train.astype(jnp.bfloat16)
    pieces = [arrange(a, tp_count) for a in (gate_round, up_round, down_round)]
    units = pieces[0].shape[1]
    moved = lax.all_to_all(
        jnp.concatenate(pieces, axis=1), "tp", split_axis=0, concat_axis=0, tiled=True
    )

    expert = (lax.axis_index("tp") // slices).astype(jnp.int32).reshape(1)
    routes_t = routes.T
    weights_t = route_weights.T
    rows, width = tokens.shape
    chosen = pl.pallas_call(
        choose_kernel,
        out_shape=jax.ShapeDtypeStruct((CAP, width), jnp.bfloat16),
        in_specs=[
            pl.BlockSpec(memory_space=pltpu.SMEM),
            pl.BlockSpec(memory_space=pltpu.VMEM),
            pl.BlockSpec(memory_space=pltpu.VMEM),
        ],
        out_specs=pl.BlockSpec(memory_space=pltpu.VMEM),
        cost_estimate=pl.CostEstimate(flops=2000000000, bytes_accessed=2000000, transcendentals=0),
        compiler_params=pltpu.CompilerParams(vmem_limit_bytes=24 * 2**20),
    )(expert, tokens, routes_t)

    block_rows = tp_count * units
    quarter = block_rows // 4
    grouped = jnp.stack(
        [
            moved[:, m * units : (m + 1) * units].reshape(4, quarter, features)
            for m in range(3)
        ],
        axis=1,
    )
    shift = (4 - lax.axis_index("fs") % 4) % 4
    turned = lax.dynamic_slice_in_dim(jnp.concatenate([grouped, grouped], axis=0), shift, 4, 0)
    packed = jnp.concatenate([turned[p] for p in range(4)], axis=-1)
    lanes = 4 * features

    wide = packed.astype(jnp.float32)
    largest = jnp.max(jnp.abs(wide), axis=(1, 2))
    factor = jnp.ones_like(largest)
    power = jnp.zeros_like(largest)
    for b in STEPS:
        fits = largest * factor * 2.0**b <= 32768.0
        factor = jnp.where(fits, factor * 2.0**b, factor)
        power = jnp.where(fits, power + b, power)
    sent = (wide * factor[:, None, None]).astype(jnp.float16).reshape(3 * quarter, lanes)
    note = jnp.broadcast_to(power[:, None], (3, lanes // 3)).reshape(1, lanes)
    note = jnp.broadcast_to(note, (8, lanes)).astype(jnp.float16)
    gathered = lax.all_gather(jnp.concatenate([sent, note], axis=0), "fs", axis=0)
    left = jnp.stack(
        [gathered[:, 3 * quarter, m * (lanes // 3)] for m in range(3)], axis=1
    ).astype(jnp.float32)
    back = jnp.ones_like(left)
    for b in STEPS:
        holds = left >= b
        back = jnp.where(holds, back * 2.0**-b, back)
        left = jnp.where(holds, left - b, left)

    def returned(start, stop):
        part = gathered[:, start * quarter : stop * quarter].astype(jnp.float32)
        part = part.reshape(fs_count, stop - start, quarter, lanes)
        part = (part * back[:, start:stop, None, None]).astype(jnp.bfloat16)
        return part.reshape(fs_count, (stop - start) * quarter, lanes)

    both = returned(0, 2)
    third = returned(2, 3)
    steps = fs_count // 4
    whole = pl.BlockSpec(memory_space=pltpu.VMEM)
    matrix = jax.ShapeDtypeStruct((block_rows, width), jnp.bfloat16)
    held = pl.BlockSpec((block_rows, lanes), lambda i: (0, jnp.minimum(i, steps - 1)))
    gate_new, up_new, partial = pl.pallas_call(
        product_kernel,
        grid=(2 * steps,),
        out_shape=(matrix, matrix, jax.ShapeDtypeStruct((width, CAP), jnp.bfloat16)),
        in_specs=[whole] * 3,
        out_specs=(
            held,
            held,
            pl.BlockSpec((lanes, CAP), lambda i: (jnp.maximum(i - steps, 0), 0)),
        ),
        scratch_shapes=[
            pltpu.VMEM((block_rows, lanes), jnp.bfloat16),
            pltpu.VMEM((CAP, block_rows), jnp.bfloat16),
            pltpu.VMEM((CAP, block_rows), jnp.float32),
            pltpu.VMEM((CAP, block_rows), jnp.float32),
        ],
        compiler_params=pltpu.CompilerParams(vmem_limit_bytes=24 * 2**20),
        cost_estimate=pl.CostEstimate(
            flops=3 * 2 * CAP * block_rows * width, bytes_accessed=2**23, transcendentals=0
        ),
    )(both, third, chosen)
    down_new = pl.pallas_call(
        output_kernel,
        grid=(steps,),
        out_shape=matrix,
        in_specs=[whole],
        out_specs=pl.BlockSpec((block_rows, lanes), lambda i: (0, i)),
        compiler_params=pltpu.CompilerParams(vmem_limit_bytes=24 * 2**20),
        cost_estimate=pl.CostEstimate(
            flops=5000000000, bytes_accessed=2**24, transcendentals=0
        ),
    )(third)

    received = lax.all_to_all(
        partial.reshape(tp_count, width // tp_count, CAP),
        "tp",
        split_axis=0,
        concat_axis=0,
        tiled=True,
    )
    mixed = pl.pallas_call(
        combine_kernel,
        out_shape=jax.ShapeDtypeStruct((width // tp_count, rows), jnp.bfloat16),
        compiler_params=pltpu.CompilerParams(vmem_limit_bytes=24 * 2**20),
    )(received, routes_t, weights_t)
    return (gate_new[None], up_new[None], down_new[None], mixed.T)


def solution(mesh):
    in_specs = (
        P("fs", None),
        P(None, "fs", "tp"),
        P(None, "fs", "tp"),
        P(None, "fs", "tp"),
        P("fs"),
        P("fs", None),
        P("fs", None),
    )
    out_specs = (P("tp", None, None), P("tp", None, None), P("tp", None, None), P("fs", "tp"))
    return jax.shard_map(shards, mesh=mesh, in_specs=in_specs, out_specs=out_specs, check_vma=False)
```

```python
import jax
import jax.numpy as jnp
from jax import lax
from jax.experimental import pallas as pl
from jax.experimental.pallas import tpu as pltpu
from jax.sharding import PartitionSpec as P

CAP = 72
EPS = 1e-06
STEPS = (56, 28, 14, 8, 4, 2, 1)
LAST = (((1,), (1,)), ((), ()))


def arrange(matrix, tp_count):
    experts, rows, cols = matrix.shape
    slices = tp_count // experts
    turned = matrix.transpose(0, 2, 1)
    return turned.reshape(tp_count, cols // slices, rows)


def ranks(routes_t, experts):
    rows = routes_t.shape[1]
    labels = lax.broadcasted_iota(jnp.int32, (experts, rows), 0)
    first = routes_t[0:1, :] == labels
    second = routes_t[1:2, :] == labels
    member = jnp.where(first | second, 1.0, 0.0)
    before = lax.broadcasted_iota(jnp.int32, (rows, rows), 0) < lax.broadcasted_iota(
        jnp.int32, (rows, rows), 1
    )
    earlier = jnp.where(before, 1.0, 0.0).astype(jnp.bfloat16)
    rank = jnp.dot(member.astype(jnp.bfloat16), earlier, preferred_element_type=jnp.float32)
    return member, rank


def choose_kernel(expert_ref, tokens_ref, routes_ref, chosen_ref):
    wide = tokens_ref[...].astype(jnp.float32)
    scale = lax.rsqrt(jnp.mean(wide * wide, axis=1, keepdims=True) + EPS)
    normed = (wide * scale).astype(jnp.bfloat16)
    rows = wide.shape[0]
    member, rank = ranks(routes_ref[...], 8)
    own = lax.broadcasted_iota(jnp.int32, member.shape, 0) == expert_ref[0]
    marked = jnp.where(own & (member > 0.5), rank, -1.0)
    place = jnp.sum(jnp.where(own, marked, 0.0), axis=0, keepdims=True)
    slots = lax.broadcasted_iota(jnp.int32, (CAP, rows), 0).astype(jnp.float32)
    picker = jnp.where(slots == place, 1.0, 0.0).astype(jnp.bfloat16)
    chosen_ref[...] = jnp.dot(picker, normed, preferred_element_type=jnp.float32).astype(
        jnp.bfloat16
    )


def by_lane(parts, shift):
    lanes = parts[0].shape[1]
    place = lax.broadcasted_iota(jnp.int32, parts[0].shape, 1)
    merged = parts[(3 - shift) % 4]
    for p in (2, 1, 0):
        merged = jnp.where(place < (p + 1) * (lanes // 4), parts[(p - shift) % 4], merged)
    return merged


def unpack(block_ref, matrix, out_ref):
    rows = out_ref.shape[0] // 4
    lanes = out_ref.shape[1]
    width = lanes // 4
    notes = [block_ref[s, 3 * rows : 3 * rows + 8, :].astype(jnp.float32) for s in range(4)]
    left = by_lane([note[matrix : matrix + 1, :] for note in notes], 0)
    back = jnp.ones_like(left)
    for b in STEPS:
        holds = left >= b
        back = jnp.where(holds, back * 2.0**-b, back)
        left = jnp.where(holds, left - b, left)
    back = back.astype(jnp.bfloat16)
    parts = [block_ref[s, matrix * rows : (matrix + 1) * rows, :] for s in range(4)]
    for g in range(4):
        merged = by_lane(parts, g)
        if g:
            merged = jnp.concatenate([merged[:, g * width :], merged[:, : g * width]], axis=1)
        out_ref[g * rows : (g + 1) * rows, :] = merged * back


def product_kernel(
    blocks_ref,
    chosen_ref,
    gate_ref,
    up_ref,
    down_ref,
    partial_ref,
    hidden_ref,
    gate_sum,
    up_sum,
    turned_ref,
):
    i = pl.program_id(0)
    steps = blocks_ref.shape[0] // 4
    lanes = gate_ref.shape[1]

    @pl.when(i < steps)
    def _():
        unpack(blocks_ref.at[pl.ds(4 * i, 4)], 0, gate_ref)
        unpack(blocks_ref.at[pl.ds(4 * i, 4)], 1, up_ref)
        chosen = chosen_ref[:, pl.ds(pl.multiple_of(i * lanes, 128), lanes)]
        gate = lax.dot_general(chosen, gate_ref[...], LAST, preferred_element_type=jnp.float32)
        up = lax.dot_general(chosen, up_ref[...], LAST, preferred_element_type=jnp.float32)

        @pl.when(i == 0)
        def _():
            gate_sum[...] = gate
            up_sum[...] = up

        @pl.when(i > 0)
        def _():
            gate_sum[...] += gate
            up_sum[...] += up

    @pl.when(i == steps - 1)
    def _():
        total = gate_sum[...]
        hidden_ref[...] = (total / (1.0 + jnp.exp(-total)) * up_sum[...]).astype(jnp.bfloat16)

    @pl.when(i >= steps)
    def _():
        j = i - steps
        unpack(blocks_ref.at[pl.ds(4 * j, 4)], 2, down_ref)
        product = jnp.dot(hidden_ref[...], down_ref[...], preferred_element_type=jnp.float32)
        turned_ref[pl.ds(pl.multiple_of(j * lanes, 128), lanes), :] = product.T

    @pl.when(i == 2 * steps - 1)
    def _():
        third = partial_ref.shape[1]
        for d in range(partial_ref.shape[0]):
            pieces = [
                turned_ref[(3 * d + g) * third : (3 * d + g + 1) * third, :] for g in range(3)
            ]
            partial_ref[d] = jnp.concatenate(pieces, axis=1).astype(jnp.bfloat16)


def combine_kernel(received_ref, routes_ref, weights_ref, mixed_ref):
    experts = 8
    slices = received_ref.shape[0] // experts
    routes = routes_ref[...]
    rows = routes.shape[1]
    _, rank = ranks(routes, experts)
    width = 3 * received_ref.shape[1]
    slots = lax.broadcasted_iota(jnp.int32, (CAP, rows), 0).astype(jnp.float32)
    totals = [jnp.zeros((width, rows), jnp.float32) for _ in range(2)]
    for e in range(experts):
        beside = received_ref[e * slices].astype(jnp.float32)
        for s in range(1, slices):
            beside = beside + received_ref[e * slices + s].astype(jnp.float32)
        summed = jnp.concatenate(
            [beside[:, g * CAP : (g + 1) * CAP] for g in range(3)], axis=0
        )
        high = summed.astype(jnp.bfloat16)
        low = (summed - high.astype(jnp.float32)).astype(jnp.bfloat16)
        at = slots == rank[e : e + 1, :]
        for j in range(2):
            named = routes[j : j + 1, :] == e
            pick = jnp.where(at & named, 1.0, 0.0).astype(jnp.bfloat16)
            totals[j] = (
                totals[j]
                + jnp.dot(high, pick, preferred_element_type=jnp.float32)
                + jnp.dot(low, pick, preferred_element_type=jnp.float32)
            )
    weights = weights_ref[...]
    mixed_ref[...] = (weights[0:1, :] * totals[0] + weights[1:2, :] * totals[1]).astype(
        jnp.bfloat16
    )


def shards(tokens, gate_train, up_train, down_train, gain, routes, route_weights):
    tp_count = lax.axis_size("tp")
    fs_count = lax.axis_size("fs")
    experts, features, _ = gate_train.shape
    slices = tp_count // experts
    gain_column = gain[None, :, None]
    gate_round = (gate_train * gain_column).astype(jnp.bfloat16)
    up_round = (up_train * gain_column).astype(jnp.bfloat16)
    down_round = down_train.astype(jnp.bfloat16)
    pieces = [arrange(a, tp_count) for a in (gate_round, up_round, down_round)]
    units = pieces[0].shape[1]
    moved = lax.all_to_all(
        jnp.concatenate(pieces, axis=1), "tp", split_axis=0, concat_axis=0, tiled=True
    )

    expert = (lax.axis_index("tp") // slices).astype(jnp.int32).reshape(1)
    routes_t = routes.T
    weights_t = route_weights.T
    rows, width = tokens.shape
    chosen = pl.pallas_call(
        choose_kernel,
        out_shape=jax.ShapeDtypeStruct((CAP, width), jnp.bfloat16),
        in_specs=[
            pl.BlockSpec(memory_space=pltpu.SMEM),
            pl.BlockSpec(memory_space=pltpu.VMEM),
            pl.BlockSpec(memory_space=pltpu.VMEM),
        ],
        out_specs=pl.BlockSpec(memory_space=pltpu.VMEM),
        cost_estimate=pl.CostEstimate(flops=2000000000, bytes_accessed=2000000, transcendentals=0),
        compiler_params=pltpu.CompilerParams(vmem_limit_bytes=24 * 2**20),
    )(expert, tokens, routes_t)

    block_rows = tp_count * units
    quarter = block_rows // 4
    grouped = jnp.stack(
        [
            moved[:, m * units : (m + 1) * units].reshape(4, quarter, features)
            for m in range(3)
        ],
        axis=1,
    )
    shift = (4 - lax.axis_index("fs") % 4) % 4
    turned = lax.dynamic_slice_in_dim(jnp.concatenate([grouped, grouped], axis=0), shift, 4, 0)
    packed = jnp.concatenate([turned[p] for p in range(4)], axis=-1)
    lanes = 4 * features

    wide = packed.astype(jnp.float32)
    largest = jnp.max(jnp.abs(wide), axis=(1, 2))
    factor = jnp.ones_like(largest)
    power = jnp.zeros_like(largest)
    for b in STEPS:
        fits = largest * factor * 2.0**b <= 32768.0
        factor = jnp.where(fits, factor * 2.0**b, factor)
        power = jnp.where(fits, power + b, power)
    sent = (wide * factor[:, None, None]).astype(jnp.float16).reshape(3 * quarter, lanes)
    note = jnp.concatenate([power, jnp.zeros((5,), jnp.float32)])
    note = jnp.broadcast_to(note[:, None], (8, lanes)).astype(jnp.float16)
    gathered = lax.all_gather(jnp.concatenate([sent, note], axis=0), "fs", axis=0)
    blocks = gathered.astype(jnp.bfloat16)
    steps = fs_count // 4
    whole = pl.BlockSpec(memory_space=pltpu.VMEM)
    matrix = jax.ShapeDtypeStruct((block_rows, width), jnp.bfloat16)
    early = pl.BlockSpec((block_rows, lanes), lambda i: (0, jnp.minimum(i, steps - 1)))
    late = pl.BlockSpec((block_rows, lanes), lambda i: (0, jnp.maximum(i - steps, 0)))
    third = width // tp_count // 3
    gate_new, up_new, down_new, partial = pl.pallas_call(
        product_kernel,
        grid=(2 * steps,),
        out_shape=(
            matrix,
            matrix,
            matrix,
            jax.ShapeDtypeStruct((tp_count, third, 3 * CAP), jnp.bfloat16),
        ),
        in_specs=[whole] * 2,
        out_specs=(early, early, late, whole),
        scratch_shapes=[
            pltpu.VMEM((CAP, block_rows), jnp.bfloat16),
            pltpu.VMEM((CAP, block_rows), jnp.float32),
            pltpu.VMEM((CAP, block_rows), jnp.float32),
            pltpu.VMEM((width, CAP), jnp.float32),
        ],
        compiler_params=pltpu.CompilerParams(vmem_limit_bytes=24 * 2**20),
        cost_estimate=pl.CostEstimate(
            flops=3 * 2 * CAP * block_rows * width, bytes_accessed=2**23, transcendentals=0
        ),
    )(blocks, chosen)
    received = lax.all_to_all(partial, "tp", split_axis=0, concat_axis=0, tiled=True)
    mixed = pl.pallas_call(
        combine_kernel,
        out_shape=jax.ShapeDtypeStruct((width // tp_count, rows), jnp.bfloat16),
        compiler_params=pltpu.CompilerParams(vmem_limit_bytes=24 * 2**20),
    )(received, routes_t, weights_t)
    return (gate_new[None], up_new[None], down_new[None], mixed.T)


def solution(mesh):
    in_specs = (
        P("fs", None),
        P(None, "fs", "tp"),
        P(None, "fs", "tp"),
        P(None, "fs", "tp"),
        P("fs"),
        P("fs", None),
        P("fs", None),
    )
    out_specs = (P("tp", None, None), P("tp", None, None), P("tp", None, None), P("fs", "tp"))
    return jax.shard_map(shards, mesh=mesh, in_specs=in_specs, out_specs=out_specs, check_vma=False)
```

```python
import jax
import jax.numpy as jnp
from jax import lax
from jax.experimental import pallas as pl
from jax.experimental.pallas import tpu as pltpu
from jax.sharding import PartitionSpec as P

CAP = 72
EPS = 1e-06
STEPS = (56, 28, 14, 8, 4, 2, 1)
LAST = (((1,), (1,)), ((), ()))


def arrange_kernel(gate_hbm, up_hbm, down_hbm, gain_ref, out_ref, held, arrived):
    _, experts, units, _ = held.shape
    slices = out_ref.shape[0] // experts
    part = units // slices
    half = experts // 2
    copies = []
    for h in range(2):
        for m, source in enumerate((gate_hbm, up_hbm, down_hbm)):
            chosen = pl.ds(h * half, half)
            copy = pltpu.make_async_copy(
                source.at[chosen], held.at[m, chosen], arrived.at[h, m]
            )
            copy.start()
            copies.append(copy)
    gain = gain_ref[...]
    for e in range(experts):
        if e % half == 0:
            for copy in copies[3 * (e // half) : 3 * (e // half) + 3]:
                copy.wait()
        for s in range(slices):
            rows = slice(s * part, (s + 1) * part)
            pieces = [held[0, e, rows, :] * gain, held[1, e, rows, :] * gain, held[2, e, rows, :]]
            out_ref[e * slices + s] = jnp.concatenate(pieces, axis=0).astype(jnp.bfloat16)


def ranks(routes_t, experts):
    rows = routes_t.shape[1]
    labels = lax.broadcasted_iota(jnp.int32, (experts, rows), 0)
    first = routes_t[0:1, :] == labels
    second = routes_t[1:2, :] == labels
    member = jnp.where(first | second, 1.0, 0.0)
    before = lax.broadcasted_iota(jnp.int32, (rows, rows), 0) < lax.broadcasted_iota(
        jnp.int32, (rows, rows), 1
    )
    earlier = jnp.where(before, 1.0, 0.0).astype(jnp.bfloat16)
    rank = jnp.dot(member.astype(jnp.bfloat16), earlier, preferred_element_type=jnp.float32)
    return member, rank


def choose_kernel(expert_ref, tokens_ref, routes_ref, chosen_ref):
    wide = tokens_ref[...].astype(jnp.float32)
    scale = lax.rsqrt(jnp.mean(wide * wide, axis=1, keepdims=True) + EPS)
    normed = (wide * scale).astype(jnp.bfloat16)
    rows = wide.shape[0]
    member, rank = ranks(routes_ref[...], 8)
    own = lax.broadcasted_iota(jnp.int32, member.shape, 0) == expert_ref[0]
    marked = jnp.where(own & (member > 0.5), rank, -1.0)
    place = jnp.sum(jnp.where(own, marked, 0.0), axis=0, keepdims=True)
    slots = lax.broadcasted_iota(jnp.int32, (CAP, rows), 0).astype(jnp.float32)
    picker = jnp.where(slots == place, 1.0, 0.0).astype(jnp.bfloat16)
    chosen_ref[...] = jnp.dot(picker, normed, preferred_element_type=jnp.float32).astype(
        jnp.bfloat16
    )


def pack_kernel(place_ref, moved_ref, out_ref, held):
    sources, units, _ = moved_ref.shape
    part = units // 3
    rows = held.shape[2]
    each = sources // 4
    largest = [None] * 3
    for g in range(4):
        wide = [moved_ref[g * each + c].astype(jnp.float32) for c in range(each)]
        for m in range(3):
            group = jnp.concatenate([w[m * part : (m + 1) * part, :] for w in wide], axis=0)
            held[m, g] = group
            top = jnp.max(jnp.max(jnp.abs(group), axis=0, keepdims=True), axis=1, keepdims=True)
            largest[m] = top if g == 0 else jnp.maximum(largest[m], top)
    factors = []
    note = jnp.zeros((8, out_ref.shape[1]), jnp.float32)
    line = lax.broadcasted_iota(jnp.int32, note.shape, 0)
    for m in range(3):
        factor = jnp.ones((1, 1), jnp.float32)
        power = jnp.zeros((1, 1), jnp.float32)
        for b in STEPS:
            fits = largest[m] * factor * 2.0**b <= 32768.0
            factor = jnp.where(fits, factor * 2.0**b, factor)
            power = jnp.where(fits, power + b, power)
        factors.append(factor)
        note = jnp.where(line == m, power, note)
    out_ref[3 * rows : 3 * rows + 8, :] = note.astype(jnp.bfloat16)
    for v in range(4):

        @pl.when(place_ref[0] == v)
        def _():
            for m in range(3):
                beside = jnp.concatenate([held[m, (p - v) % 4] for p in range(4)], axis=1)
                out_ref[m * rows : (m + 1) * rows, :] = (beside * factors[m]).astype(jnp.bfloat16)


def scales(blocks_ref, back_ref):
    lanes = blocks_ref.shape[2]
    width = lanes // 4
    first = blocks_ref.shape[1] - 8
    place = lax.broadcasted_iota(jnp.int32, (8, lanes), 1)
    for i in range(blocks_ref.shape[0] // 4):
        notes = [blocks_ref[4 * i + s, first:, :].astype(jnp.float32) for s in range(4)]
        left = notes[3]
        for s in (2, 1, 0):
            left = jnp.where(place < (s + 1) * width, notes[s], left)
        back = jnp.ones_like(left)
        for b in STEPS:
            holds = left >= b
            back = jnp.where(holds, back * 2.0**-b, back)
            left = jnp.where(holds, left - b, left)
        back_ref[:, i * lanes : (i + 1) * lanes] = back


def unpack(block_ref, matrix, back, out_ref, start):
    rows = out_ref.shape[0] // 4
    lane = lax.broadcasted_iota(jnp.int32, (rows, 128), 1)
    below = {n: lane < n for n in (32, 64, 96)}
    back = back.astype(jnp.bfloat16)
    tiles = [
        [
            block_ref[s, matrix * rows : (matrix + 1) * rows, 128 * t : 128 * (t + 1)]
            for t in range(3)
        ]
        for s in range(4)
    ]
    for g in range(4):
        merged = [
            jnp.where(below[96 - 32 * t], tiles[(t - g) % 4][t], tiles[(t + 1 - g) % 4][t])
            for t in range(3)
        ]
        if g:
            skip, by = divmod(96 * g, 128)
            turned = [jnp.concatenate([m[:, by:], m[:, :by]], axis=1) for m in merged]
            merged = [
                jnp.where(below[128 - by], turned[(t + skip) % 3], turned[(t + skip + 1) % 3])
                for t in range(3)
            ]
        for t in range(3):
            out_ref[
                g * rows : (g + 1) * rows, start + 128 * t : start + 128 * (t + 1)
            ] = merged[t] * back[:, 128 * t : 128 * (t + 1)]


def product_kernel(
    blocks_ref,
    chosen_ref,
    gate_ref,
    up_ref,
    down_ref,
    partial_ref,
    hidden_ref,
    gate_sum,
    up_sum,
    turned_ref,
    back_ref,
):
    i = pl.program_id(0)
    steps = pl.num_programs(0) // 2
    lanes = blocks_ref.shape[2]
    wide = gate_ref.shape[1]
    inner = wide // lanes

    @pl.when(i == 0)
    def _():
        scales(blocks_ref, back_ref)

    def place(step, matrix, out_ref):
        columns = pl.ds(pl.multiple_of(step * wide, 128), wide)
        back = back_ref[:, columns]
        for n in range(inner):
            unpack(
                blocks_ref.at[pl.ds(4 * (step * inner + n), 4)],
                matrix,
                back[matrix : matrix + 1, n * lanes : (n + 1) * lanes],
                out_ref,
                n * lanes,
            )

    @pl.when(i < steps)
    def _():
        place(i, 0, gate_ref)
        place(i, 1, up_ref)
        chosen = chosen_ref[:, pl.ds(pl.multiple_of(i * wide, 128), wide)]
        gate = lax.dot_general(chosen, gate_ref[...], LAST, preferred_element_type=jnp.float32)
        up = lax.dot_general(chosen, up_ref[...], LAST, preferred_element_type=jnp.float32)

        @pl.when(i == 0)
        def _():
            gate_sum[...] = gate
            up_sum[...] = up

        @pl.when(i > 0)
        def _():
            gate_sum[...] += gate
            up_sum[...] += up

    @pl.when(i == steps - 1)
    def _():
        total = gate_sum[...]
        hidden_ref[...] = (total / (1.0 + jnp.exp(-total)) * up_sum[...]).astype(jnp.bfloat16)

    @pl.when(i >= steps)
    def _():
        j = i - steps
        place(j, 2, down_ref)
        product = jnp.dot(hidden_ref[...], down_ref[...], preferred_element_type=jnp.float32)
        turned_ref[pl.ds(pl.multiple_of(j * wide, 128), wide), :] = product.T

    @pl.when(i == 2 * steps - 1)
    def _():
        third = partial_ref.shape[1]
        for d in range(partial_ref.shape[0]):
            pieces = [
                turned_ref[(3 * d + g) * third : (3 * d + g + 1) * third, :] for g in range(3)
            ]
            partial_ref[d] = jnp.concatenate(pieces, axis=1).astype(jnp.bfloat16)


def combine_kernel(received_ref, routes_ref, weights_ref, mixed_ref):
    experts = 8
    slices = received_ref.shape[0] // experts
    routes = routes_ref[...]
    rows = routes.shape[1]
    _, rank = ranks(routes, experts)
    width = 3 * received_ref.shape[1]
    slots = lax.broadcasted_iota(jnp.int32, (CAP, rows), 0).astype(jnp.float32)
    totals = [jnp.zeros((width, rows), jnp.float32) for _ in range(2)]
    for e in range(experts):
        beside = received_ref[e * slices].astype(jnp.float32)
        for s in range(1, slices):
            beside = beside + received_ref[e * slices + s].astype(jnp.float32)
        summed = jnp.concatenate(
            [beside[:, g * CAP : (g + 1) * CAP] for g in range(3)], axis=0
        )
        high = summed.astype(jnp.bfloat16)
        low = (summed - high.astype(jnp.float32)).astype(jnp.bfloat16)
        at = slots == rank[e : e + 1, :]
        for j in range(2):
            named = routes[j : j + 1, :] == e
            pick = jnp.where(at & named, 1.0, 0.0).astype(jnp.bfloat16)
            totals[j] = (
                totals[j]
                + jnp.dot(high, pick, preferred_element_type=jnp.float32)
                + jnp.dot(low, pick, preferred_element_type=jnp.float32)
            )
    weights = weights_ref[...]
    mixed_ref[...] = (weights[0:1, :] * totals[0] + weights[1:2, :] * totals[1]).astype(
        jnp.bfloat16
    )


def shards(tokens, gate_train, up_train, down_train, gain, routes, route_weights):
    tp_count = lax.axis_size("tp")
    fs_count = lax.axis_size("fs")
    experts, features, _ = gate_train.shape
    slices = tp_count // experts
    units = gate_train.shape[2] // slices
    moved = lax.all_to_all(
        pl.pallas_call(
            arrange_kernel,
            out_shape=jax.ShapeDtypeStruct((tp_count, 3 * units, features), jnp.bfloat16),
            in_specs=[pl.BlockSpec(memory_space=pltpu.MemorySpace.HBM)] * 3
            + [pl.BlockSpec(memory_space=pltpu.VMEM)],
            scratch_shapes=[
                pltpu.VMEM((3, experts, slices * units, features), jnp.float32),
                pltpu.SemaphoreType.DMA((2, 3)),
            ],
            compiler_params=pltpu.CompilerParams(vmem_limit_bytes=60 * 1024 * 2**10),
        )(
            gate_train.transpose(0, 2, 1),
            up_train.transpose(0, 2, 1),
            down_train.transpose(0, 2, 1),
            gain[None, :],
        ),
        "tp",
        split_axis=0,
        concat_axis=0,
        tiled=True,
    )

    expert = (lax.axis_index("tp") // slices).astype(jnp.int32).reshape(1)
    routes_t = routes.T
    weights_t = route_weights.T
    rows, width = tokens.shape
    chosen = pl.pallas_call(
        choose_kernel,
        out_shape=jax.ShapeDtypeStruct((CAP, width), jnp.bfloat16),
        in_specs=[
            pl.BlockSpec(memory_space=pltpu.SMEM),
            pl.BlockSpec(memory_space=pltpu.VMEM),
            pl.BlockSpec(memory_space=pltpu.VMEM),
        ],
        out_specs=pl.BlockSpec(memory_space=pltpu.VMEM),
        cost_estimate=pl.CostEstimate(flops=2000000000, bytes_accessed=2000000, transcendentals=0),
        compiler_params=pltpu.CompilerParams(vmem_limit_bytes=24 * 2**20),
    )(expert, tokens, routes_t)

    block_rows = tp_count * units
    quarter = block_rows // 4
    lanes = 4 * features
    packed = pl.pallas_call(
        pack_kernel,
        out_shape=jax.ShapeDtypeStruct((3 * quarter + 8, lanes), jnp.bfloat16),
        in_specs=[
            pl.BlockSpec(memory_space=pltpu.SMEM),
            pl.BlockSpec(memory_space=pltpu.VMEM),
        ],
        out_specs=pl.BlockSpec(memory_space=pltpu.VMEM),
        scratch_shapes=[pltpu.VMEM((3, 4, quarter, features), jnp.float32)],
        compiler_params=pltpu.CompilerParams(vmem_limit_bytes=24 * 2**20),
    )((lax.axis_index("fs") % 4).astype(jnp.int32).reshape(1), moved)
    gathered = lax.all_gather(packed.astype(jnp.float16), "fs", axis=0)
    blocks = gathered.astype(jnp.bfloat16)
    steps = fs_count // 8
    wide = width // steps
    whole = pl.BlockSpec(memory_space=pltpu.VMEM)
    matrix = jax.ShapeDtypeStruct((block_rows, width), jnp.bfloat16)
    early = pl.BlockSpec((block_rows, wide), lambda i: (0, jnp.minimum(i, steps - 1)))
    late = pl.BlockSpec((block_rows, wide), lambda i: (0, jnp.maximum(i - steps, 0)))
    third = width // tp_count // 3
    gate_new, up_new, down_new, partial = pl.pallas_call(
        product_kernel,
        grid=(2 * steps,),
        out_shape=(
            matrix,
            matrix,
            matrix,
            jax.ShapeDtypeStruct((tp_count, third, 3 * CAP), jnp.bfloat16),
        ),
        in_specs=[whole] * 2,
        out_specs=(early, early, late, whole),
        scratch_shapes=[
            pltpu.VMEM((CAP, block_rows), jnp.bfloat16),
            pltpu.VMEM((CAP, block_rows), jnp.float32),
            pltpu.VMEM((CAP, block_rows), jnp.float32),
            pltpu.VMEM((width, CAP), jnp.float32),
            pltpu.VMEM((8, width), jnp.float32),
        ],
        compiler_params=pltpu.CompilerParams(vmem_limit_bytes=24 * 2**20),
        cost_estimate=pl.CostEstimate(
            flops=3 * 2 * CAP * block_rows * width, bytes_accessed=2**23, transcendentals=0
        ),
    )(blocks, chosen)
    received = lax.all_to_all(partial, "tp", split_axis=0, concat_axis=0, tiled=True)
    mixed = pl.pallas_call(
        combine_kernel,
        out_shape=jax.ShapeDtypeStruct((width // tp_count, rows), jnp.bfloat16),
        compiler_params=pltpu.CompilerParams(vmem_limit_bytes=24 * 2**20),
    )(received, routes_t, weights_t)
    return (gate_new[None], up_new[None], down_new[None], mixed.T)


def solution(mesh):
    in_specs = (
        P("fs", None),
        P(None, "fs", "tp"),
        P(None, "fs", "tp"),
        P(None, "fs", "tp"),
        P("fs"),
        P("fs", None),
        P("fs", None),
    )
    out_specs = (P("tp", None, None), P("tp", None, None), P("tp", None, None), P("fs", "tp"))
    return jax.shard_map(shards, mesh=mesh, in_specs=in_specs, out_specs=out_specs, check_vma=False)
```

```python
import jax
import jax.numpy as jnp
from jax import lax
from jax.experimental import pallas as pl
from jax.experimental.pallas import tpu as pltpu
from jax.sharding import PartitionSpec as P

CAP = 72
EPS = 1e-06
STEPS = (56, 28, 14, 8, 4, 2, 1)
LAST = (((1,), (1,)), ((), ()))


def arrange_kernel(gate_hbm, up_hbm, down_hbm, gain_ref, out_ref, held, arrived):
    _, experts, units, _ = held.shape
    slices = out_ref.shape[0] // experts
    part = units // slices
    half = experts // 2
    copies = []
    for h in range(2):
        for m, source in enumerate((gate_hbm, up_hbm, down_hbm)):
            chosen = pl.ds(h * half, half)
            copy = pltpu.make_async_copy(
                source.at[chosen], held.at[m, chosen], arrived.at[h, m]
            )
            copy.start()
            copies.append(copy)
    gain = gain_ref[...]
    features = gain.shape[1]
    rest = 128 - features
    gap = jnp.zeros((2, rest), jnp.float32)
    for e in range(experts):
        if e % half == 0:
            for copy in copies[3 * (e // half) : 3 * (e // half) + 3]:
                copy.wait()
        for s in range(slices):
            rows = slice(s * part, (s + 1) * part)
            pieces = [held[0, e, rows, :] * gain, held[1, e, rows, :] * gain, held[2, e, rows, :]]
            lines = jnp.concatenate(pieces, axis=0)
            beside = []
            for q in range(3):
                beside += [lines[48:54, q * rest : (q + 1) * rest], gap]
            upper = jnp.concatenate([lines[0:24], jnp.concatenate(beside, axis=0)], axis=1)
            lower = jnp.concatenate([lines[24:48], jnp.zeros((24, rest), jnp.float32)], axis=1)
            out_ref[e * slices + s] = jnp.concatenate([upper, lower], axis=0).astype(jnp.bfloat16)


def ranks(routes_t, experts):
    rows = routes_t.shape[1]
    labels = lax.broadcasted_iota(jnp.int32, (experts, rows), 0)
    first = routes_t[0:1, :] == labels
    second = routes_t[1:2, :] == labels
    member = jnp.where(first | second, 1.0, 0.0)
    before = lax.broadcasted_iota(jnp.int32, (rows, rows), 0) < lax.broadcasted_iota(
        jnp.int32, (rows, rows), 1
    )
    earlier = jnp.where(before, 1.0, 0.0).astype(jnp.bfloat16)
    rank = jnp.dot(member.astype(jnp.bfloat16), earlier, preferred_element_type=jnp.float32)
    return member, rank


def choose_kernel(expert_ref, tokens_ref, routes_ref, chosen_ref):
    wide = tokens_ref[...].astype(jnp.float32)
    scale = lax.rsqrt(jnp.mean(wide * wide, axis=1, keepdims=True) + EPS)
    normed = (wide * scale).astype(jnp.bfloat16)
    rows = wide.shape[0]
    member, rank = ranks(routes_ref[...], 8)
    own = lax.broadcasted_iota(jnp.int32, member.shape, 0) == expert_ref[0]
    marked = jnp.where(own & (member > 0.5), rank, -1.0)
    place = jnp.sum(jnp.where(own, marked, 0.0), axis=0, keepdims=True)
    slots = lax.broadcasted_iota(jnp.int32, (CAP, rows), 0).astype(jnp.float32)
    picker = jnp.where(slots == place, 1.0, 0.0).astype(jnp.bfloat16)
    chosen_ref[...] = jnp.dot(picker, normed, preferred_element_type=jnp.float32).astype(
        jnp.bfloat16
    )


def pack_kernel(place_ref, moved_ref, out_ref, held):
    sources = moved_ref.shape[0]
    rows, features = held.shape[2:]
    part = 4 * rows // sources
    each = sources // 4
    largest = [None] * 3
    for g in range(4):
        wide = [moved_ref[g * each + c].astype(jnp.float32) for c in range(each)]
        for m in range(3):
            pieces = []
            for w in wide:
                pieces.append(w[m * part : min((m + 1) * part, 48), 0:features])
                if m == 2:
                    tail = [w[8 * q : 8 * q + 6, features:] for q in range(3)]
                    pieces.append(jnp.concatenate(tail, axis=1))
            group = jnp.concatenate(pieces, axis=0)
            held[m, g] = group
            top = jnp.max(jnp.max(jnp.abs(group), axis=0, keepdims=True), axis=1, keepdims=True)
            largest[m] = top if g == 0 else jnp.maximum(largest[m], top)
    factors = []
    note = jnp.zeros((8, out_ref.shape[1]), jnp.float32)
    line = lax.broadcasted_iota(jnp.int32, note.shape, 0)
    for m in range(3):
        factor = jnp.ones((1, 1), jnp.float32)
        power = jnp.zeros((1, 1), jnp.float32)
        for b in STEPS:
            fits = largest[m] * factor * 2.0**b <= 32768.0
            factor = jnp.where(fits, factor * 2.0**b, factor)
            power = jnp.where(fits, power + b, power)
        factors.append(factor)
        note = jnp.where(line == m, power, note)
    out_ref[3 * rows : 3 * rows + 8, :] = note.astype(jnp.bfloat16)
    for v in range(4):

        @pl.when(place_ref[0] == v)
        def _():
            for m in range(3):
                beside = jnp.concatenate([held[m, (p - v) % 4] for p in range(4)], axis=1)
                out_ref[m * rows : (m + 1) * rows, :] = (beside * factors[m]).astype(jnp.bfloat16)


def scales(blocks_ref, back_ref):
    lanes = blocks_ref.shape[2]
    width = lanes // 4
    first = blocks_ref.shape[1] - 8
    place = lax.broadcasted_iota(jnp.int32, (8, lanes), 1)
    for i in range(blocks_ref.shape[0] // 4):
        notes = [blocks_ref[4 * i + s, first:, :].astype(jnp.float32) for s in range(4)]
        left = notes[3]
        for s in (2, 1, 0):
            left = jnp.where(place < (s + 1) * width, notes[s], left)
        back = jnp.ones_like(left)
        for b in STEPS:
            holds = left >= b
            back = jnp.where(holds, back * 2.0**-b, back)
            left = jnp.where(holds, left - b, left)
        back_ref[:, i * lanes : (i + 1) * lanes] = back


def unpack(block_ref, matrix, back, out_ref, start):
    rows = out_ref.shape[0] // 4
    lane = lax.broadcasted_iota(jnp.int32, (rows, 128), 1)
    below = {n: lane < n for n in (32, 64, 96)}
    back = back.astype(jnp.bfloat16)
    tiles = [
        [
            block_ref[s, matrix * rows : (matrix + 1) * rows, 128 * t : 128 * (t + 1)]
            for t in range(3)
        ]
        for s in range(4)
    ]
    for g in range(4):
        merged = [
            jnp.where(below[96 - 32 * t], tiles[(t - g) % 4][t], tiles[(t + 1 - g) % 4][t])
            for t in range(3)
        ]
        if g:
            skip, by = divmod(96 * g, 128)
            turned = [jnp.concatenate([m[:, by:], m[:, :by]], axis=1) for m in merged]
            merged = [
                jnp.where(below[128 - by], turned[(t + skip) % 3], turned[(t + skip + 1) % 3])
                for t in range(3)
            ]
        for t in range(3):
            out_ref[
                g * rows : (g + 1) * rows, start + 128 * t : start + 128 * (t + 1)
            ] = merged[t] * back[:, 128 * t : 128 * (t + 1)]


def product_kernel(
    blocks_ref,
    chosen_ref,
    gate_hbm,
    up_hbm,
    down_hbm,
    partial_ref,
    held,
    gate_sum,
    up_sum,
    result_ref,
    back_ref,
    written,
):
    steps = written.shape[1]
    lanes = blocks_ref.shape[2]
    wide = held.shape[2] // steps
    inner = wide // lanes
    outputs = (gate_hbm, up_hbm, down_hbm)
    copies = []
    scales(blocks_ref, back_ref)

    def place(step, matrix):
        for n in range(inner):
            at = step * wide + n * lanes
            unpack(
                blocks_ref.at[pl.ds(4 * (step * inner + n), 4)],
                matrix,
                back_ref[matrix : matrix + 1, at : at + lanes],
                held.at[matrix],
                at,
            )

    def write(step, matrix):
        columns = pl.ds(step * wide, wide)
        copy = pltpu.make_async_copy(
            held.at[matrix, :, columns], outputs[matrix].at[:, columns], written.at[matrix, step]
        )
        copy.start()
        copies.append(copy)

    for i in range(steps):
        columns = slice(i * wide, (i + 1) * wide)
        place(i, 0)
        place(i, 1)
        chosen = chosen_ref[:, columns]
        for matrix, total in ((0, gate_sum), (1, up_sum)):
            part = lax.dot_general(
                chosen, held[matrix, :, columns], LAST, preferred_element_type=jnp.float32
            )
            if i:
                total[...] += part
            else:
                total[...] = part
        write(i, 0)
        write(i, 1)
    gate = gate_sum[...]
    hidden = (gate / (1.0 + jnp.exp(-gate)) * up_sum[...]).astype(jnp.bfloat16)
    for i in range(steps):
        columns = slice(i * wide, (i + 1) * wide)
        place(i, 2)
        result_ref[:, columns] = jnp.dot(
            hidden, held[2, :, columns], preferred_element_type=jnp.float32
        )
        write(i, 2)

    third = partial_ref.shape[1]
    own = partial_ref.shape[2] // 3
    for d in range(partial_ref.shape[0]):
        pieces = [
            result_ref[g * third : (g + 1) * third, d * own : (d + 1) * own] for g in range(3)
        ]
        partial_ref[d] = jnp.concatenate(pieces, axis=1).astype(jnp.bfloat16)
    for copy in copies:
        copy.wait()


def combine_kernel(received_ref, routes_ref, weights_ref, mixed_ref):
    experts = 8
    slices = received_ref.shape[0] // experts
    routes = routes_ref[...]
    rows = routes.shape[1]
    _, rank = ranks(routes, experts)
    width = received_ref.shape[2] // 3
    slots = lax.broadcasted_iota(jnp.int32, (CAP, rows), 0).astype(jnp.float32)
    totals = [jnp.zeros((width, rows), jnp.float32) for _ in range(2)]
    for e in range(experts):
        beside = received_ref[e * slices].astype(jnp.float32)
        for s in range(1, slices):
            beside = beside + received_ref[e * slices + s].astype(jnp.float32)
        summed = jnp.concatenate(
            [beside[:, g * width : (g + 1) * width] for g in range(3)], axis=0
        ).T
        high = summed.astype(jnp.bfloat16)
        low = (summed - high.astype(jnp.float32)).astype(jnp.bfloat16)
        at = slots == rank[e : e + 1, :]
        for j in range(2):
            named = routes[j : j + 1, :] == e
            pick = jnp.where(at & named, 1.0, 0.0).astype(jnp.bfloat16)
            totals[j] = (
                totals[j]
                + jnp.dot(high, pick, preferred_element_type=jnp.float32)
                + jnp.dot(low, pick, preferred_element_type=jnp.float32)
            )
    weights = weights_ref[...]
    mixed_ref[...] = (weights[0:1, :] * totals[0] + weights[1:2, :] * totals[1]).astype(
        jnp.bfloat16
    )


def shards(tokens, gate_train, up_train, down_train, gain, routes, route_weights):
    tp_count = lax.axis_size("tp")
    fs_count = lax.axis_size("fs")
    experts, features, _ = gate_train.shape
    slices = tp_count // experts
    units = gate_train.shape[2] // slices
    moved = lax.all_to_all(
        pl.pallas_call(
            arrange_kernel,
            out_shape=jax.ShapeDtypeStruct((tp_count, 48, 128), jnp.bfloat16),
            in_specs=[pl.BlockSpec(memory_space=pltpu.MemorySpace.HBM)] * 3
            + [pl.BlockSpec(memory_space=pltpu.VMEM)],
            scratch_shapes=[
                pltpu.VMEM((3, experts, slices * units, features), jnp.float32),
                pltpu.SemaphoreType.DMA((2, 3)),
            ],
            compiler_params=pltpu.CompilerParams(vmem_limit_bytes=60 * 1024 * 2**10),
        )(
            gate_train.transpose(0, 2, 1),
            up_train.transpose(0, 2, 1),
            down_train.transpose(0, 2, 1),
            gain[None, :],
        ),
        "tp",
        split_axis=0,
        concat_axis=0,
        tiled=True,
    )

    expert = (lax.axis_index("tp") // slices).astype(jnp.int32).reshape(1)
    routes_t = routes.T
    weights_t = route_weights.T
    rows, width = tokens.shape
    chosen = pl.pallas_call(
        choose_kernel,
        out_shape=jax.ShapeDtypeStruct((CAP, width), jnp.bfloat16),
        in_specs=[
            pl.BlockSpec(memory_space=pltpu.SMEM),
            pl.BlockSpec(memory_space=pltpu.VMEM),
            pl.BlockSpec(memory_space=pltpu.VMEM),
        ],
        out_specs=pl.BlockSpec(memory_space=pltpu.VMEM),
        cost_estimate=pl.CostEstimate(flops=2000000000, bytes_accessed=2000000, transcendentals=0),
        compiler_params=pltpu.CompilerParams(vmem_limit_bytes=24 * 2**20),
    )(expert, tokens, routes_t)

    block_rows = tp_count * units
    quarter = block_rows // 4
    lanes = 4 * features
    packed = pl.pallas_call(
        pack_kernel,
        out_shape=jax.ShapeDtypeStruct((3 * quarter + 8, lanes), jnp.bfloat16),
        in_specs=[
            pl.BlockSpec(memory_space=pltpu.SMEM),
            pl.BlockSpec(memory_space=pltpu.VMEM),
        ],
        out_specs=pl.BlockSpec(memory_space=pltpu.VMEM),
        scratch_shapes=[pltpu.VMEM((3, 4, quarter, features), jnp.float32)],
        compiler_params=pltpu.CompilerParams(vmem_limit_bytes=24 * 2**20),
    )((lax.axis_index("fs") % 4).astype(jnp.int32).reshape(1), moved)
    gathered = lax.all_gather(packed.astype(jnp.float16), "fs", axis=0)
    blocks = gathered.astype(jnp.bfloat16)
    steps = fs_count // 8
    wide = width // steps
    whole = pl.BlockSpec(memory_space=pltpu.VMEM)
    matrix = jax.ShapeDtypeStruct((block_rows, width), jnp.bfloat16)
    far = pl.BlockSpec(memory_space=pltpu.MemorySpace.HBM)
    own_width = width // tp_count
    gate_new, up_new, down_new, partial = pl.pallas_call(
        product_kernel,
        out_shape=(
            matrix,
            matrix,
            matrix,
            jax.ShapeDtypeStruct((tp_count, CAP // 3, 3 * own_width), jnp.bfloat16),
        ),
        in_specs=[whole] * 2,
        out_specs=(far, far, far, whole),
        scratch_shapes=[
            pltpu.VMEM((3, block_rows, width), jnp.bfloat16),
            pltpu.VMEM((CAP, block_rows), jnp.float32),
            pltpu.VMEM((CAP, block_rows), jnp.float32),
            pltpu.VMEM((CAP, width), jnp.float32),
            pltpu.VMEM((8, width), jnp.float32),
            pltpu.SemaphoreType.DMA((3, steps)),
        ],
        compiler_params=pltpu.CompilerParams(vmem_limit_bytes=24 * 2**20),
        cost_estimate=pl.CostEstimate(
            flops=3 * 2 * CAP * block_rows * width, bytes_accessed=2**23, transcendentals=0
        ),
    )(blocks, chosen)
    received = lax.all_to_all(partial, "tp", split_axis=0, concat_axis=0, tiled=True)
    mixed = pl.pallas_call(
        combine_kernel,
        out_shape=jax.ShapeDtypeStruct((width // tp_count, rows), jnp.bfloat16),
        compiler_params=pltpu.CompilerParams(vmem_limit_bytes=24 * 2**20),
    )(received, routes_t, weights_t)
    return (gate_new[None], up_new[None], down_new[None], mixed.T)


def solution(mesh):
    in_specs = (
        P("fs", None),
        P(None, "fs", "tp"),
        P(None, "fs", "tp"),
        P(None, "fs", "tp"),
        P("fs"),
        P("fs", None),
        P("fs", None),
    )
    out_specs = (P("tp", None, None), P("tp", None, None), P("tp", None, None), P("fs", "tp"))
    return jax.shard_map(shards, mesh=mesh, in_specs=in_specs, out_specs=out_specs, check_vma=False)
```

```python
import jax
import jax.numpy as jnp
from jax import lax
from jax.experimental import pallas as pl
from jax.experimental.pallas import tpu as pltpu
from jax.sharding import PartitionSpec as P

CAP = 72
EPS = 1e-06
STEPS = (56, 28, 14, 8, 4, 2, 1)
LAST = (((1,), (1,)), ((), ()))


def arrange_kernel(gate_hbm, up_hbm, down_hbm, gain_ref, out_ref, held, arrived):
    _, experts, units, _ = held.shape
    slices = out_ref.shape[0] // experts
    part = units // slices
    few = experts // 4
    copies = []
    for h in range(4):
        for m, source in enumerate((gate_hbm, up_hbm, down_hbm)):
            chosen = pl.ds(h * few, few)
            copy = pltpu.make_async_copy(
                source.at[chosen], held.at[m, chosen], arrived.at[h, m]
            )
            copy.start()
            copies.append(copy)
    gain = gain_ref[...]
    features = gain.shape[1]
    rest = 128 - features
    gap = jnp.zeros((2, rest), jnp.float32)
    for e in range(experts):
        if e % few == 0:
            for copy in copies[3 * (e // few) : 3 * (e // few) + 3]:
                copy.wait()
        for s in range(slices):
            rows = slice(s * part, (s + 1) * part)
            pieces = [held[0, e, rows, :] * gain, held[1, e, rows, :] * gain, held[2, e, rows, :]]
            lines = jnp.concatenate(pieces, axis=0)
            beside = []
            for q in range(3):
                beside += [lines[48:54, q * rest : (q + 1) * rest], gap]
            upper = jnp.concatenate([lines[0:24], jnp.concatenate(beside, axis=0)], axis=1)
            lower = jnp.concatenate([lines[24:48], jnp.zeros((24, rest), jnp.float32)], axis=1)
            out_ref[e * slices + s] = jnp.concatenate([upper, lower], axis=0).astype(jnp.bfloat16)


def ranks(routes_t, experts):
    rows = routes_t.shape[1]
    labels = lax.broadcasted_iota(jnp.int32, (experts, rows), 0)
    first = routes_t[0:1, :] == labels
    second = routes_t[1:2, :] == labels
    member = jnp.where(first | second, 1.0, 0.0)
    before = lax.broadcasted_iota(jnp.int32, (rows, rows), 0) < lax.broadcasted_iota(
        jnp.int32, (rows, rows), 1
    )
    earlier = jnp.where(before, 1.0, 0.0).astype(jnp.bfloat16)
    rank = jnp.dot(member.astype(jnp.bfloat16), earlier, preferred_element_type=jnp.float32)
    return member, rank


def choose_kernel(expert_ref, tokens_ref, routes_ref, chosen_ref):
    wide = tokens_ref[...].astype(jnp.float32)
    scale = lax.rsqrt(jnp.mean(wide * wide, axis=1, keepdims=True) + EPS)
    normed = (wide * scale).astype(jnp.bfloat16)
    rows = wide.shape[0]
    member, rank = ranks(routes_ref[...], 8)
    own = lax.broadcasted_iota(jnp.int32, member.shape, 0) == expert_ref[0]
    marked = jnp.where(own & (member > 0.5), rank, -1.0)
    place = jnp.sum(jnp.where(own, marked, 0.0), axis=0, keepdims=True)
    slots = lax.broadcasted_iota(jnp.int32, (CAP, rows), 0).astype(jnp.float32)
    picker = jnp.where(slots == place, 1.0, 0.0).astype(jnp.bfloat16)
    chosen_ref[...] = jnp.dot(picker, normed, preferred_element_type=jnp.float32).astype(
        jnp.bfloat16
    )


def pack_kernel(place_ref, moved_ref, out_ref, held):
    sources = moved_ref.shape[0]
    rows, features = held.shape[2:]
    part = 4 * rows // sources
    each = sources // 4
    largest = [None] * 3
    for g in range(4):
        wide = [moved_ref[g * each + c].astype(jnp.float32) for c in range(each)]
        for m in range(3):
            pieces = []
            for w in wide:
                pieces.append(w[m * part : min((m + 1) * part, 48), 0:features])
                if m == 2:
                    tail = [w[8 * q : 8 * q + 6, features:] for q in range(3)]
                    pieces.append(jnp.concatenate(tail, axis=1))
            group = jnp.concatenate(pieces, axis=0)
            held[m, g] = group
            top = jnp.max(jnp.max(jnp.abs(group), axis=0, keepdims=True), axis=1, keepdims=True)
            largest[m] = top if g == 0 else jnp.maximum(largest[m], top)
    factors = []
    note = jnp.zeros((8, out_ref.shape[1]), jnp.float32)
    line = lax.broadcasted_iota(jnp.int32, note.shape, 0)
    for m in range(3):
        factor = jnp.ones((1, 1), jnp.float32)
        power = jnp.zeros((1, 1), jnp.float32)
        for b in STEPS:
            fits = largest[m] * factor * 2.0**b <= 32768.0
            factor = jnp.where(fits, factor * 2.0**b, factor)
            power = jnp.where(fits, power + b, power)
        factors.append(factor)
        note = jnp.where(line == m, power, note)
    out_ref[3 * rows : 3 * rows + 8, :] = note.astype(jnp.bfloat16)
    for v in range(4):

        @pl.when(place_ref[0] == v)
        def _():
            for m in range(3):
                beside = jnp.concatenate([held[m, (p - v) % 4] for p in range(4)], axis=1)
                out_ref[m * rows : (m + 1) * rows, :] = (beside * factors[m]).astype(jnp.bfloat16)


def scales(blocks_ref, back_ref):
    lanes = blocks_ref.shape[2]
    width = lanes // 4
    first = blocks_ref.shape[1] - 8
    place = lax.broadcasted_iota(jnp.int32, (8, lanes), 1)
    for i in range(blocks_ref.shape[0] // 4):
        notes = [blocks_ref[4 * i + s, first:, :].astype(jnp.float32) for s in range(4)]
        left = notes[3]
        for s in (2, 1, 0):
            left = jnp.where(place < (s + 1) * width, notes[s], left)
        back = jnp.ones_like(left)
        for b in STEPS:
            holds = left >= b
            back = jnp.where(holds, back * 2.0**-b, back)
            left = jnp.where(holds, left - b, left)
        back_ref[:, i * lanes : (i + 1) * lanes] = back


def unpack(block_ref, matrix, back, out_ref, start):
    rows = out_ref.shape[0] // 4
    lane = lax.broadcasted_iota(jnp.int32, (rows, 128), 1)
    below = {n: lane < n for n in (32, 64, 96)}
    back = back.astype(jnp.bfloat16)
    tiles = [
        [
            block_ref[s, matrix * rows : (matrix + 1) * rows, 128 * t : 128 * (t + 1)]
            for t in range(3)
        ]
        for s in range(4)
    ]
    for g in range(4):
        merged = [
            jnp.where(below[96 - 32 * t], tiles[(t - g) % 4][t], tiles[(t + 1 - g) % 4][t])
            for t in range(3)
        ]
        if g:
            skip, by = divmod(96 * g, 128)
            turned = [jnp.concatenate([m[:, by:], m[:, :by]], axis=1) for m in merged]
            merged = [
                jnp.where(below[128 - by], turned[(t + skip) % 3], turned[(t + skip + 1) % 3])
                for t in range(3)
            ]
        for t in range(3):
            out_ref[
                g * rows : (g + 1) * rows, start + 128 * t : start + 128 * (t + 1)
            ] = merged[t] * back[:, 128 * t : 128 * (t + 1)]


def product_kernel(
    blocks_ref,
    chosen_ref,
    gate_hbm,
    up_hbm,
    down_hbm,
    partial_ref,
    held,
    gate_sum,
    up_sum,
    result_ref,
    back_ref,
    written,
):
    steps = written.shape[1]
    lanes = blocks_ref.shape[2]
    wide = held.shape[2] // steps
    inner = wide // lanes
    outputs = (gate_hbm, up_hbm, down_hbm)
    copies = []
    scales(blocks_ref, back_ref)

    def place(step, matrix):
        for n in range(inner):
            at = step * wide + n * lanes
            unpack(
                blocks_ref.at[pl.ds(4 * (step * inner + n), 4)],
                matrix,
                back_ref[matrix : matrix + 1, at : at + lanes],
                held.at[matrix],
                at,
            )

    def write(step, matrix):
        columns = pl.ds(step * wide, wide)
        copy = pltpu.make_async_copy(
            held.at[matrix, :, columns], outputs[matrix].at[:, columns], written.at[matrix, step]
        )
        copy.start()
        copies.append(copy)

    for i in range(steps):
        columns = slice(i * wide, (i + 1) * wide)
        place(i, 0)
        place(i, 1)
        chosen = chosen_ref[:, columns]
        for matrix, total in ((0, gate_sum), (1, up_sum)):
            part = lax.dot_general(
                chosen, held[matrix, :, columns], LAST, preferred_element_type=jnp.float32
            )
            if i:
                total[...] += part
            else:
                total[...] = part
        write(i, 0)
        write(i, 1)
    gate = gate_sum[...]
    hidden = (gate / (1.0 + jnp.exp(-gate)) * up_sum[...]).astype(jnp.bfloat16)
    for i in range(steps):
        columns = slice(i * wide, (i + 1) * wide)
        place(i, 2)
        result_ref[:, columns] = jnp.dot(
            hidden, held[2, :, columns], preferred_element_type=jnp.float32
        )
        write(i, 2)

    third = partial_ref.shape[1]
    own = partial_ref.shape[2] // 3
    for d in range(partial_ref.shape[0]):
        pieces = [
            result_ref[g * third : (g + 1) * third, d * own : (d + 1) * own] for g in range(3)
        ]
        partial_ref[d] = jnp.concatenate(pieces, axis=1).astype(jnp.bfloat16)
    for copy in copies:
        copy.wait()


def combine_kernel(received_ref, routes_ref, weights_ref, mixed_ref):
    experts = 8
    slices = received_ref.shape[0] // experts
    routes = routes_ref[...]
    rows = routes.shape[1]
    _, rank = ranks(routes, experts)
    width = received_ref.shape[2] // 3
    slots = lax.broadcasted_iota(jnp.int32, (CAP, rows), 0).astype(jnp.float32)
    totals = [jnp.zeros((width, rows), jnp.float32) for _ in range(2)]
    for e in range(experts):
        beside = received_ref[e * slices].astype(jnp.float32)
        for s in range(1, slices):
            beside = beside + received_ref[e * slices + s].astype(jnp.float32)
        summed = jnp.concatenate(
            [beside[:, g * width : (g + 1) * width] for g in range(3)], axis=0
        ).T
        high = summed.astype(jnp.bfloat16)
        low = (summed - high.astype(jnp.float32)).astype(jnp.bfloat16)
        at = slots == rank[e : e + 1, :]
        for j in range(2):
            named = routes[j : j + 1, :] == e
            pick = jnp.where(at & named, 1.0, 0.0).astype(jnp.bfloat16)
            totals[j] = (
                totals[j]
                + jnp.dot(high, pick, preferred_element_type=jnp.float32)
                + jnp.dot(low, pick, preferred_element_type=jnp.float32)
            )
    weights = weights_ref[...]
    mixed_ref[...] = (weights[0:1, :] * totals[0] + weights[1:2, :] * totals[1]).astype(
        jnp.bfloat16
    )


def shards(tokens, gate_train, up_train, down_train, gain, routes, route_weights):
    tp_count = lax.axis_size("tp")
    fs_count = lax.axis_size("fs")
    experts, features, _ = gate_train.shape
    slices = tp_count // experts
    units = gate_train.shape[2] // slices
    moved = lax.all_to_all(
        pl.pallas_call(
            arrange_kernel,
            out_shape=jax.ShapeDtypeStruct((tp_count, 48, 128), jnp.bfloat16),
            in_specs=[pl.BlockSpec(memory_space=pltpu.MemorySpace.HBM)] * 3
            + [pl.BlockSpec(memory_space=pltpu.VMEM)],
            scratch_shapes=[
                pltpu.VMEM((3, experts, slices * units, features), jnp.float32),
                pltpu.SemaphoreType.DMA((4, 3)),
            ],
            compiler_params=pltpu.CompilerParams(vmem_limit_bytes=60 * 1024 * 2**10),
        )(
            gate_train.transpose(0, 2, 1),
            up_train.transpose(0, 2, 1),
            down_train.transpose(0, 2, 1),
            gain[None, :],
        ),
        "tp",
        split_axis=0,
        concat_axis=0,
        tiled=True,
    )

    expert = (lax.axis_index("tp") // slices).astype(jnp.int32).reshape(1)
    routes_t = routes.T
    weights_t = route_weights.T
    rows, width = tokens.shape
    chosen = pl.pallas_call(
        choose_kernel,
        out_shape=jax.ShapeDtypeStruct((CAP, width), jnp.bfloat16),
        in_specs=[
            pl.BlockSpec(memory_space=pltpu.SMEM),
            pl.BlockSpec(memory_space=pltpu.VMEM),
            pl.BlockSpec(memory_space=pltpu.VMEM),
        ],
        out_specs=pl.BlockSpec(memory_space=pltpu.VMEM),
        cost_estimate=pl.CostEstimate(flops=2000000000, bytes_accessed=2000000, transcendentals=0),
        compiler_params=pltpu.CompilerParams(vmem_limit_bytes=24 * 2**20),
    )(expert, tokens, routes_t)

    block_rows = tp_count * units
    quarter = block_rows // 4
    lanes = 4 * features
    packed = pl.pallas_call(
        pack_kernel,
        out_shape=jax.ShapeDtypeStruct((3 * quarter + 8, lanes), jnp.bfloat16),
        in_specs=[
            pl.BlockSpec(memory_space=pltpu.SMEM),
            pl.BlockSpec(memory_space=pltpu.VMEM),
        ],
        out_specs=pl.BlockSpec(memory_space=pltpu.VMEM),
        scratch_shapes=[pltpu.VMEM((3, 4, quarter, features), jnp.float32)],
        compiler_params=pltpu.CompilerParams(vmem_limit_bytes=24 * 2**20),
    )((lax.axis_index("fs") % 4).astype(jnp.int32).reshape(1), moved)
    gathered = lax.all_gather(packed.astype(jnp.float16), "fs", axis=0)
    blocks = gathered.astype(jnp.bfloat16)
    steps = fs_count // 8
    wide = width // steps
    whole = pl.BlockSpec(memory_space=pltpu.VMEM)
    matrix = jax.ShapeDtypeStruct((block_rows, width), jnp.bfloat16)
    far = pl.BlockSpec(memory_space=pltpu.MemorySpace.HBM)
    own_width = width // tp_count
    gate_new, up_new, down_new, partial = pl.pallas_call(
        product_kernel,
        out_shape=(
            matrix,
            matrix,
            matrix,
            jax.ShapeDtypeStruct((tp_count, CAP // 3, 3 * own_width), jnp.bfloat16),
        ),
        in_specs=[whole] * 2,
        out_specs=(far, far, far, whole),
        scratch_shapes=[
            pltpu.VMEM((3, block_rows, width), jnp.bfloat16),
            pltpu.VMEM((CAP, block_rows), jnp.float32),
            pltpu.VMEM((CAP, block_rows), jnp.float32),
            pltpu.VMEM((CAP, width), jnp.float32),
            pltpu.VMEM((8, width), jnp.float32),
            pltpu.SemaphoreType.DMA((3, steps)),
        ],
        compiler_params=pltpu.CompilerParams(vmem_limit_bytes=24 * 2**20),
        cost_estimate=pl.CostEstimate(
            flops=3 * 2 * CAP * block_rows * width, bytes_accessed=2**23, transcendentals=0
        ),
    )(blocks, chosen)
    received = lax.all_to_all(partial, "tp", split_axis=0, concat_axis=0, tiled=True)
    mixed = pl.pallas_call(
        combine_kernel,
        out_shape=jax.ShapeDtypeStruct((width // tp_count, rows), jnp.bfloat16),
        compiler_params=pltpu.CompilerParams(vmem_limit_bytes=24 * 2**20),
    )(received, routes_t, weights_t)
    return (gate_new[None], up_new[None], down_new[None], mixed.T)


def solution(mesh):
    in_specs = (
        P("fs", None),
        P(None, "fs", "tp"),
        P(None, "fs", "tp"),
        P(None, "fs", "tp"),
        P("fs"),
        P("fs", None),
        P("fs", None),
    )
    out_specs = (P("tp", None, None), P("tp", None, None), P("tp", None, None), P("fs", "tp"))
    return jax.shard_map(shards, mesh=mesh, in_specs=in_specs, out_specs=out_specs, check_vma=False)
```
